256 devices in a mesh: sp: 32 (over z, y), tp: 8 (over x, core).
Axes of the slice: x: 4, y: 4, z: 8, core: 2. Of those that a mesh axis runs over, the one named last changes fastest.
Arguments:
- tokens: bfloat16 [16384, 2048], P('sp', 'tp'), may hold values from -6 to 6
- in_gain: float32 [2048], replicated, may hold values from 0.1 to 1.9
- conv_value_w: bfloat16 [2048, 1024], P(None, 'tp'), may hold values from -0.125 to 0.125
- conv_gate_w: bfloat16 [2048, 1024], P(None, 'tp'), may hold values from -0.125 to 0.125
- conv_taps: float32 [31, 1024], P(None, 'tp'), may hold values from -8 to 8
- conv_gain: float32 [1024], P('tp'), may hold values from 0.1 to 1.9
- query_latent_weight: bfloat16 [2048, 512], replicated, may hold values from -0.125 to 0.125
- latent_weight: bfloat16 [2048, 512], replicated, may hold values from -0.125 to 0.125
- rope_key_w: bfloat16 [2048, 64], replicated, may hold values from -0.125 to 0.125
- query_gain: float32 [512], replicated, may hold values from 1.5 to 8, as said below
- latent_gain: float32 [512], replicated, may hold values from 1.5 to 8, as said below
- query_weight: bfloat16 [512, 1024], P(None, 'tp'), may hold values from -0.25 to 0.25
- query_rotary_weight: bfloat16 [512, 512], P(None, 'tp'), may hold values from -0.25 to 0.25
- key_weight: bfloat16 [512, 1024], P(None, 'tp'), may hold values from -0.25 to 0.25
- value_weight: bfloat16 [512, 1024], P(None, 'tp'), may hold values from -0.25 to 0.25
- conv_out_w: bfloat16 [1024, 2048], P('tp'), may hold values from -0.125 to 0.125
- attn_out_w: bfloat16 [1024, 2048], P('tp'), may hold values from -0.125 to 0.125
- out_gain: float32 [2048], replicated, may hold values from 0.1 to 1.9
Outputs:
- mixed: bfloat16 [16384, 2048], P(('sp', 'tp'))
The draws below stay inside these ranges and needn't reach their ends.
Inputs may be any that keep to these rules, and one draw needn't show every extreme that they name: `query_gain`: positive gains. `latent_gain`: positive gains.
All inputs are finite; a program needn't handle non-finite values.
Results may differ from the reference program's by a relative error of at most 0.018.
The reference program's roundings to bfloat16 on the way count: a program that leaves them out, or rounds other values in their place, can miss the bound.
Values may be sent and summed in bfloat16 or wider, within the bound.
No kernel may reach another device: no remote copies, remote signals or barrier semaphores. Data moves between devices by JAX's collectives and lax.ppermute only.
A program may use at most 128 MiB of HBM per device.

```python
import math
import jax
import jax.numpy as jnp
from jax import lax

MODEL_WIDTH = 2048
CONV_CH = 1024
CONV_K = 31
HALF_K = 15
HEAD_COUNT = 8
HEAD_WIDTH = 128
ROTARY_WIDTH = 64
QUERY_LATENT = 512
LATENT_WIDTH = 512
TOKENS = 16384
N_TP = 8


def draw_conv_taps(key, part):
    first_key, second_key = jax.random.split(jax.random.fold_in(key, 11))
    channel_place = jnp.arange(CONV_CH, dtype=jnp.float32) / CONV_CH
    jitter = jax.random.uniform(first_key, (CONV_CH,), jnp.float32)
    exponent = 0.5 * channel_place + 0.5 * jitter
    base = jnp.clip(jax.random.normal(second_key, (CONV_K, CONV_CH), jnp.float32), -4.0, 4.0)
    return base * CONV_K ** (-0.5) * (10.0 ** exponent)[None, :]


def draw_gain_vector(key, width):
    jitter = jax.random.uniform(key, (width,), jnp.float32)
    lower, upper = (1.5, 3.0)
    return jnp.exp(jnp.log(lower) + jitter * (jnp.log(upper) - jnp.log(lower)))


def draw_query_gain(key, part):
    return draw_gain_vector(jax.random.fold_in(key, 23), QUERY_LATENT)


def draw_latent_gain(key, part):
    return draw_gain_vector(jax.random.fold_in(key, 37), LATENT_WIDTH)


def block_levels(own_key, dims, cuts, low, high):
    loudness = 1.0
    for position, shards_of in cuts:
        draws = jax.random.uniform(jax.random.fold_in(jax.random.fold_in(own_key, 6), position), (shards_of,), jnp.float32, low / len(cuts), high / len(cuts))
        loudness = loudness * jnp.repeat(jnp.exp(draws), dims[position] // shards_of).reshape((-1,) + (1,) * (len(dims) - 1 - position))
    return loudness


def bell_draw(rng, shape, spread, reach, shards=(), held_as=jnp.bfloat16):
    entries = spread * jax.random.normal(rng, shape, jnp.float32)
    if shards:
        entries = entries * block_levels(rng, shape, shards, -0.22, 0.18)
    return jnp.clip(entries, -reach, reach).astype(held_as)


def setup_inputs(seed: int = 0) -> dict:
    splits = jax.random.split(jax.random.key(seed), 19)
    tokens = bell_draw(splits[0], (TOKENS, MODEL_WIDTH), 1.0, 6.0, ((0, 32), (1, 8)))
    in_gain = jnp.clip(1.0 + 0.18 * jax.random.normal(splits[1], (MODEL_WIDTH,), jnp.float32), 0.1, 1.9)
    conv_value_w = bell_draw(splits[2], (MODEL_WIDTH, CONV_CH), MODEL_WIDTH ** -0.5, 0.125, ((1, 8),))
    conv_gate_w = bell_draw(splits[3], (MODEL_WIDTH, CONV_CH), MODEL_WIDTH ** -0.5, 0.125, ((1, 8),))
    conv_taps = draw_conv_taps(jax.random.fold_in(splits[18], 71), 0)
    conv_gain = jnp.clip(1.0 + 0.18 * jax.random.normal(splits[5], (CONV_CH,), jnp.float32), 0.1, 1.9)
    query_latent_weight = bell_draw(splits[6], (MODEL_WIDTH, QUERY_LATENT), MODEL_WIDTH ** -0.5, 0.125)
    latent_weight = bell_draw(splits[7], (MODEL_WIDTH, LATENT_WIDTH), MODEL_WIDTH ** -0.5, 0.125)
    rope_key_w = bell_draw(splits[8], (MODEL_WIDTH, ROTARY_WIDTH), MODEL_WIDTH ** -0.5, 0.125)
    query_gain = draw_query_gain(jax.random.fold_in(splits[18], 71), 0)
    latent_gain = draw_latent_gain(jax.random.fold_in(splits[18], 71), 0)
    query_weight = bell_draw(splits[11], (QUERY_LATENT, HEAD_COUNT * HEAD_WIDTH), QUERY_LATENT ** -0.5, 0.25, ((1, 8),))
    query_rotary_weight = bell_draw(splits[12], (QUERY_LATENT, HEAD_COUNT * ROTARY_WIDTH), QUERY_LATENT ** -0.5, 0.25, ((1, 8),))
    key_weight = bell_draw(splits[13], (LATENT_WIDTH, HEAD_COUNT * HEAD_WIDTH), LATENT_WIDTH ** -0.5, 0.25, ((1, 8),))
    value_weight = bell_draw(splits[14], (LATENT_WIDTH, HEAD_COUNT * HEAD_WIDTH), LATENT_WIDTH ** -0.5, 0.25, ((1, 8),))
    conv_out_w = bell_draw(splits[15], (CONV_CH, MODEL_WIDTH), (CONV_CH + HEAD_COUNT * HEAD_WIDTH) ** -0.5, 0.125, ((0, 8),))
    attn_out_w = bell_draw(splits[16], (HEAD_COUNT * HEAD_WIDTH, MODEL_WIDTH), (CONV_CH + HEAD_COUNT * HEAD_WIDTH) ** -0.5, 0.125, ((0, 8),))
    out_gain = jnp.clip(1.0 + 0.18 * jax.random.normal(splits[17], (MODEL_WIDTH,), jnp.float32), 0.1, 1.9)
    return {"tokens": tokens, "in_gain": in_gain, "conv_value_w": conv_value_w, "conv_gate_w": conv_gate_w, "conv_taps": conv_taps, "conv_gain": conv_gain, "query_latent_weight": query_latent_weight, "latent_weight": latent_weight, "rope_key_w": rope_key_w, "query_gain": query_gain, "latent_gain": latent_gain, "query_weight": query_weight, "query_rotary_weight": query_rotary_weight, "key_weight": key_weight, "value_weight": value_weight, "conv_out_w": conv_out_w, "attn_out_w": attn_out_w, "out_gain": out_gain}


norm_eps = 1e-06
layer_eps = 1e-05
rope_base = 10000.0

def to_float(values):
    return lax.optimization_barrier(values).astype(jnp.float32)

def rms_scaled(values, gain):
    return values * lax.rsqrt(lax.optimization_barrier(jnp.mean(values * values, axis=-1, keepdims=True)) + norm_eps) * gain

def rotate(values, cosine_table, sine_table):
    halfway = values.shape[-1] // 2
    first = values[..., :halfway]
    second = values[..., halfway:]
    return jnp.concatenate([first * cosine_table - second * sine_table, second * cosine_table + first * sine_table], axis=-1)

def tables(positions, width):
    halfway = width // 2
    inverse = rope_base ** (-jnp.arange(halfway, dtype=jnp.float32) / halfway)
    angles = positions[:, None] * inverse[None, :]
    return (jnp.cos(angles), jnp.sin(angles))

def reference(tokens, in_gain, conv_value_w, conv_gate_w, conv_taps, conv_gain, query_latent_weight, latent_weight, rope_key_w, query_gain, latent_gain, query_weight, query_rotary_weight, key_weight, value_weight, conv_out_w, attn_out_w, out_gain):
    tokens_all = tokens.shape[0]
    normed = rms_scaled(tokens.astype(jnp.float32), in_gain).astype(jnp.bfloat16)
    conv_value = jnp.dot(normed, conv_value_w, preferred_element_type=jnp.float32)
    conv_gate = jnp.dot(normed, conv_gate_w, preferred_element_type=jnp.float32)
    gated = (conv_value * jax.nn.sigmoid(conv_gate)).astype(jnp.bfloat16)
    padded = jnp.pad(to_float(gated), ((HALF_K, HALF_K), (0, 0)))
    convolved = jnp.zeros((tokens_all, CONV_CH), jnp.float32)
    for offset_tap in range(CONV_K):
        convolved = convolved + conv_taps[offset_tap] * padded[offset_tap:offset_tap + tokens_all]
    chan_mean = lax.optimization_barrier(jnp.mean(convolved, axis=1, keepdims=True))
    chan_square = lax.optimization_barrier(jnp.mean(convolved * convolved, axis=1, keepdims=True))
    shaped = (convolved - chan_mean) * lax.rsqrt(chan_square - chan_mean * chan_mean + layer_eps) * conv_gain
    conv_result = jax.nn.silu(shaped).astype(jnp.bfloat16)
    positions = jnp.arange(tokens_all, dtype=jnp.int32).astype(jnp.float32)
    cosine_table, sine_table = tables(positions, ROTARY_WIDTH)
    query_lat = rms_scaled(jnp.dot(normed, query_latent_weight, preferred_element_type=jnp.float32), query_gain).astype(jnp.bfloat16)
    latent = rms_scaled(jnp.dot(normed, latent_weight, preferred_element_type=jnp.float32), latent_gain).astype(jnp.bfloat16)
    rope_keys = rotate(jnp.dot(normed, rope_key_w, preferred_element_type=jnp.float32), cosine_table, sine_table).astype(jnp.bfloat16)
    query_main = jnp.dot(query_lat, query_weight, preferred_element_type=jnp.float32).astype(jnp.bfloat16).reshape(tokens_all, HEAD_COUNT, HEAD_WIDTH)
    query_rope = rotate(jnp.dot(query_lat, query_rotary_weight, preferred_element_type=jnp.float32).reshape(tokens_all, HEAD_COUNT, ROTARY_WIDTH), cosine_table[:, None, :], sine_table[:, None, :]).astype(jnp.bfloat16)
    key_float = to_float(jnp.dot(latent, key_weight, preferred_element_type=jnp.float32).astype(jnp.bfloat16)).reshape(tokens_all, HEAD_COUNT, HEAD_WIDTH)
    value_float = to_float(jnp.dot(latent, value_weight, preferred_element_type=jnp.float32).astype(jnp.bfloat16)).reshape(tokens_all, HEAD_COUNT, HEAD_WIDTH)
    rope_float = to_float(rope_keys)
    score_scale = (HEAD_WIDTH + ROTARY_WIDTH) ** (-0.5)
    query_block = math.gcd(tokens_all, 512)
    block_count = tokens_all // query_block

    def one_block(pieces):
        block_main, block_rope = pieces
        scores = (jnp.einsum('thd,khd->htk', to_float(block_main), key_float) + jnp.einsum('thr,kr->htk', to_float(block_rope), rope_float)) * score_scale
        top_score = lax.optimization_barrier(jnp.max(scores, axis=-1, keepdims=True))
        weights = jnp.exp(scores - top_score)
        totals = lax.optimization_barrier(jnp.sum(weights, axis=-1))
        summed = jnp.einsum('htk,khd->thd', to_float(weights.astype(jnp.bfloat16)), value_float)
        return (summed / totals.T[:, :, None]).astype(jnp.bfloat16)
    blocks_out = lax.map(one_block, (query_main.reshape(block_count, query_block, HEAD_COUNT, HEAD_WIDTH), query_rope.reshape(block_count, query_block, HEAD_COUNT, ROTARY_WIDTH)))
    attention_result = blocks_out.reshape(tokens_all, HEAD_COUNT * HEAD_WIDTH)
    chan_share = CONV_CH // N_TP
    head_share = HEAD_COUNT * HEAD_WIDTH // N_TP
    merged = jnp.zeros((tokens_all, MODEL_WIDTH), jnp.float32)
    for group in range(N_TP):
        partial_value = jnp.dot(conv_result[:, group * chan_share:(group + 1) * chan_share], conv_out_w[group * chan_share:(group + 1) * chan_share], preferred_element_type=jnp.float32) + jnp.dot(attention_result[:, group * head_share:(group + 1) * head_share], attn_out_w[group * head_share:(group + 1) * head_share], preferred_element_type=jnp.float32)
        merged = merged + to_float(partial_value.astype(jnp.bfloat16))
    return rms_scaled(merged, out_gain).astype(jnp.bfloat16)
```

```python
import functools

import jax
import jax.numpy as jnp
from jax import lax
from jax.experimental import pallas as pl
from jax.experimental.pallas import tpu as pltpu
from jax.sharding import Mesh, PartitionSpec as P


norm_eps = 1e-06
layer_eps = 1e-05
rope_base = 10000.0
log2_e = 1.4426950408889634

MODEL = 2048
CH = 128
ROT = 64
ROWS = 512
CONV_CH = 1024
bf16 = jnp.bfloat16
f32 = jnp.float32
VMEM_LIMIT = 56 * 1024 * 1024


def struct(shape, dtype):
    return jax.ShapeDtypeStruct(shape, dtype)


def call(body, outs, args, scratch=(), flops=0, aliases=None, smem_first=False):
    vm = pl.BlockSpec(memory_space=pltpu.VMEM)
    specs = [vm] * len(args)
    if smem_first:
        specs[0] = pl.BlockSpec(memory_space=pltpu.SMEM)
    bytes_moved = sum(a.size * a.dtype.itemsize for a in list(args) + list(outs))
    return pl.pallas_call(
        body,
        in_specs=specs,
        out_specs=[vm] * len(outs),
        out_shape=list(outs),
        scratch_shapes=list(scratch),
        input_output_aliases=aliases or {},
        cost_estimate=pl.CostEstimate(flops=flops, transcendentals=0, bytes_accessed=bytes_moved),
        compiler_params=pltpu.CompilerParams(vmem_limit_bytes=VMEM_LIMIT),
    )(*args)


def dot(a, b):
    return jnp.dot(a, b, preferred_element_type=f32)


def front_body(idx, p0, p1, p2, p3, o0, o1, o2, o3, gain, lat_w, rope_w, lat_gain, key_w, value_w, cs, sn, normed, kr, vt):
    x, c = idx[0], idx[1]
    own, other = (p0, p1, p2, p3), (o0, o1, o2, o3)
    total = jnp.zeros((ROWS, 1), f32)
    for r in own + other:
        v = r[...].astype(f32)
        total = total + jnp.sum(v * v, axis=1, keepdims=True)
    scale = lax.rsqrt(total / MODEL + norm_eps)
    for s in range(4):
        for r, core in ((own[s], c), (other[s], 1 - c)):
            at = pl.multiple_of(((x + 4 - s) % 4 * 2 + core) * 256, 256)
            normed[:, pl.ds(at, 256)] = (r[...].astype(f32) * scale * gain[:, pl.ds(at, 256)]).astype(bf16)
    n = normed[...]
    lat = dot(n, lat_w[...])
    lat = (lat * lax.rsqrt(jnp.mean(lat * lat, axis=1, keepdims=True) + norm_eps) * lat_gain[...]).astype(bf16)
    kr[0:ROWS, :] = dot(lat, key_w[...]).astype(bf16)
    vt[...] = dot(lat, value_w[...]).T.astype(bf16)
    both = dot(n, rope_w[...])
    rope = (both[:, 0:ROT] * cs[...] + both[:, ROT:] * sn[...]).astype(bf16)
    kr[ROWS:, :] = jnp.concatenate([rope[: ROWS // 2], rope[ROWS // 2 :]], axis=1)


def query_body(normed, lat_w, gain, main_w, rot_w, cs, sn, out, *, scale):
    lat = dot(normed[...], lat_w[...])
    lat = (lat * lax.rsqrt(jnp.mean(lat * lat, axis=1, keepdims=True) + norm_eps) * gain[...]).astype(bf16)
    out[0:CH, :] = (dot(lat, main_w[...]) * scale).T.astype(bf16)
    both = dot(lat, rot_w[...])
    rot = (both[:, 0:ROT] * cs[...] + both[:, ROT:] * sn[...]) * scale
    out[CH:, :] = rot.T.astype(bf16)


def gate_body(normed, value_w, gate_w, out):
    n = normed[...]
    v = dot(n, value_w[...])
    g = dot(n, gate_w[...])
    out[...] = (v * jax.nn.sigmoid(g)).astype(bf16)


def conv_body(gated, before, after, taps, out, stats, pad):
    pad[0:16, :] = before[...].astype(f32)
    pad[16 : 16 + ROWS, :] = gated[...].astype(f32)
    pad[16 + ROWS :, :] = after[...].astype(f32)
    for b in range(ROWS // 128):
        acc = jnp.zeros((128, CH), f32)
        for j in range(31):
            acc = acc + taps[j : j + 1, :] * pad[b * 128 + j + 1 : b * 128 + j + 129, :]
        t = acc.T
        out[:, b * 128 : (b + 1) * 128] = t
        stats[0:1, b * 128 : (b + 1) * 128] = jnp.sum(t, axis=0, keepdims=True)
        stats[1:2, b * 128 : (b + 1) * 128] = jnp.sum(t * t, axis=0, keepdims=True)
    stats[2:, :] = jnp.zeros((6, ROWS), f32)


def conv_end_body(conv, s0, s1, s2, s3, gain, out):
    st = s0[...] + s1[...] + s2[...] + s3[...]
    mean = st[0:1, :] / CONV_CH
    square = st[1:2, :] / CONV_CH
    shaped = (conv[...] - mean) * lax.rsqrt(square - mean * mean + layer_eps) * gain[...]
    out[...] = (shaped * jax.nn.sigmoid(shaped)).astype(bf16)


def attend_body(pieces, first, last, *refs):
    q = refs[0:4]
    kv = refs[4 : 4 + 2 * pieces]
    at = 4 + 2 * pieces
    if not first:
        m_in, l_in, a_in = refs[at : at + 3]
        at += 3
    outs = refs[at : -2]
    ks, qs = refs[-2:]
    for s in range(4):
        qs[:, s * ROWS : (s + 1) * ROWS] = q[s][...]
    for p in range(pieces):
        kr = kv[2 * p]
        ks[p * ROWS : (p + 1) * ROWS, 0:CH] = kr[0:ROWS, :]
        ks[p * ROWS : p * ROWS + 256, CH : CH + ROT] = kr[ROWS:, 0:ROT]
        ks[p * ROWS + 256 : (p + 1) * ROWS, CH : CH + ROT] = kr[ROWS:, ROT:]
    if not first:
        m, l, a = m_in[0:1, :], l_in[0:1, :], a_in[...]
    qv = qs[...]
    for p in range(pieces):
        s = dot(ks[p * ROWS : (p + 1) * ROWS, 0 : CH + ROT], qv)
        top = jnp.max(s, axis=0, keepdims=True)
        if p or not first:
            new = jnp.maximum(m, top)
            keep = jnp.exp2(m - new)
        else:
            new = top
        w = jnp.exp2(s - new)
        part = jnp.sum(w, axis=0, keepdims=True)
        pv = dot(kv[2 * p + 1][...], w.astype(bf16))
        if p or not first:
            l = l * keep + part
            a = a * keep + pv
        else:
            l, a = part, pv
        m = new
    if last:
        o = (a / l).astype(bf16)
        for s in range(4):
            sl = slice(s * ROWS, (s + 1) * ROWS)
            outs[s][...] = o[:, sl]
            outs[4 + s][...] = jnp.concatenate([m[:, sl], l[:, sl], jnp.zeros((6, ROWS), f32)], axis=0)
    else:
        n = m.shape[1]
        outs[0][...] = jnp.broadcast_to(m, (8, n))
        outs[1][...] = jnp.broadcast_to(l, (8, n))
        outs[2][...] = a


def attend(q, kv, state, last):
    pieces, first = len(kv), state is None
    n = 4 * ROWS
    if last:
        outs = [struct((CH, ROWS), bf16)] * 4 + [struct((8, ROWS), f32)] * 4
    else:
        outs = [struct((8, n), f32), struct((8, n), f32), struct((CH, n), f32)]
    args = list(q) + [a for pair in kv for a in pair] + ([] if first else list(state))
    at = 4 + 2 * pieces
    aliases = {} if first or last else {at: 0, at + 1: 1, at + 2: 2}
    return call(
        functools.partial(attend_body, pieces, first, last),
        outs,
        args,
        scratch=[pltpu.VMEM((ROWS * pieces, 256), bf16), pltpu.VMEM((CH + ROT, n), bf16)],
        flops=2 * n * ROWS * pieces * 512,
        aliases=aliases,
    )


def out_body(idx, o0, o1, o2, o3, t0, t1, t2, t3, conv, conv_w, attn_w, own, other, full):
    x, c = idx[0], idx[1]
    os, ts = (o0, o1, o2, o3), (t0, t1, t2, t3)
    top = jnp.maximum(jnp.maximum(t0[0:1, :], t1[0:1, :]), jnp.maximum(t2[0:1, :], t3[0:1, :]))
    num = jnp.zeros((CH, ROWS), f32)
    den = jnp.zeros((1, ROWS), f32)
    for o, t in zip(os, ts):
        w = t[1:2, :] * jnp.exp2(t[0:1, :] - top)
        num = num + o[...].astype(f32) * w
        den = den + w
    att = (num / den).T.astype(bf16)
    cv = conv[...].astype(f32).T.astype(bf16)
    full[...] = dot(cv, conv_w[...]) + dot(att, attn_w[...])
    for s in range(4):
        row = (x + s) % 4 * 2
        own[s * 64 : (s + 1) * 64, :] = full[pl.ds(pl.multiple_of((row + c) * 64, 64), 64), :]
        other[s * 64 : (s + 1) * 64, :] = full[pl.ds(pl.multiple_of((row + 1 - c) * 64, 64), 64), :].astype(bf16)


def pair_sum_body(own, other, s0, s1, s2, s3):
    s0[...] = own[0:64, :] + other[0:64, :].astype(f32)
    for s, r in ((1, s1), (2, s2), (3, s3)):
        r[...] = (own[s * 64 : (s + 1) * 64, :] + other[s * 64 : (s + 1) * 64, :].astype(f32)).astype(bf16)


def end_body(s0, r1, r2, r3, gain, out):
    v = s0[...] + r1[...].astype(f32) + r2[...].astype(f32) + r3[...].astype(f32)
    out[...] = (v * lax.rsqrt(jnp.mean(v * v, axis=1, keepdims=True) + norm_eps) * gain[...]).astype(bf16)


def shift(value, axis, by):
    n = lax.axis_size(axis)
    return lax.ppermute(value, axis, [(i, (i + by) % n) for i in range(n)])


def swapped(w):
    return jnp.concatenate([w, w[:, ROT // 2 :], w[:, : ROT // 2]], axis=1)


def local(
    tokens,
    in_gain,
    conv_value_w,
    conv_gate_w,
    conv_taps,
    conv_gain,
    query_latent_weight,
    latent_weight,
    rope_key_w,
    query_gain,
    latent_gain,
    query_weight,
    query_rotary_weight,
    key_weight,
    value_weight,
    conv_out_w,
    attn_out_w,
    out_gain,
):
    x, c = lax.axis_index("x"), lax.axis_index("c")
    idx = jnp.stack([x, c]).astype(jnp.int32)
    own = [tokens] + [shift(tokens, "x", s) for s in (1, 2, 3)]
    other = [shift(t, "c", 1) for t in own]

    block = lax.axis_index("z") * lax.axis_size("y") + lax.axis_index("y")
    positions = (block * ROWS + jnp.arange(ROWS, dtype=jnp.int32)).astype(f32)
    half = ROT // 2
    inverse = rope_base ** (-jnp.arange(half, dtype=f32) / half)
    angles = positions[:, None] * inverse[None, :]
    cosine, sine = jnp.cos(angles), jnp.sin(angles)
    cs = jnp.concatenate([cosine, cosine], axis=1)
    sn = jnp.concatenate([-sine, sine], axis=1)

    normed, kr, vt = call(
        front_body,
        [struct((ROWS, MODEL), bf16), struct((ROWS + ROWS // 2, CH), bf16), struct((CH, ROWS), bf16)],
        [idx, *own, *other, in_gain[None, :], latent_weight, swapped(rope_key_w), latent_gain[None, :], key_weight, value_weight, cs, sn],
        flops=2 * ROWS * MODEL * 768,
        smem_first=True,
    )
    (qt,) = call(
        functools.partial(query_body, scale=(CH + ROT) ** (-0.5) * log2_e),
        [struct((CH + ROT, ROWS), bf16)],
        [normed, query_latent_weight, query_gain[None, :], query_weight, swapped(query_rotary_weight), cs, sn],
        flops=2 * ROWS * MODEL * 640,
    )
    q = [qt] + [shift(qt, "y", s) for s in (1, 2, 3)]

    right, left = [(kr, vt)], [(kr, vt)]
    for s in range(3):
        right.append(tuple(shift(a, "z", 1) for a in right[-1]))
        left.append(tuple(shift(a, "z", -1) for a in left[-1]))
    far = (shift(right[3][0], "z", 1), shift(left[3][1], "z", -1))

    (gated,) = call(
        gate_body, [struct((ROWS, CH), bf16)], [normed, conv_value_w, conv_gate_w], flops=2 * ROWS * MODEL * 256
    )
    sp = ("z", "y")
    n_sp = lax.axis_size("z") * lax.axis_size("y")
    before = lax.ppermute(gated[ROWS - 16 :], sp, [(i, i + 1) for i in range(n_sp - 1)])
    after = lax.ppermute(gated[:16], sp, [(i + 1, i) for i in range(n_sp - 1)])
    conv, stats = call(
        conv_body,
        [struct((CH, ROWS), f32), struct((8, ROWS), f32)],
        [gated, before, after, conv_taps],
        scratch=[pltpu.VMEM((ROWS + 32, CH), f32)],
        flops=2 * ROWS * CH * 31 * 20,
    )
    stats = stats + shift(stats, "c", 1)
    (conv_result,) = call(
        conv_end_body,
        [struct((CH, ROWS), bf16)],
        [conv, stats, *[shift(stats, "x", s) for s in (1, 2, 3)], conv_gain[:, None]],
        flops=ROWS * CH * 100,
    )

    state = attend(q, [(kr, vt), right[1], left[1]], None, False)
    state = attend(q, [right[2], left[2]], state, False)
    state = attend(q, [right[3], left[3]], state, False)
    res = attend(q, [far], state, True)
    os, ts = res[:4], res[4:]
    os = [os[0]] + [shift(os[s], "y", -s) for s in (1, 2, 3)]
    ts = [ts[0]] + [shift(ts[s], "y", -s) for s in (1, 2, 3)]

    mine, theirs = call(
        out_body,
        [struct((256, MODEL), f32), struct((256, MODEL), bf16)],
        [idx, *os, *ts, conv_result, conv_out_w, attn_out_w],
        scratch=[pltpu.VMEM((ROWS, MODEL), f32)],
        flops=2 * ROWS * MODEL * 256,
        smem_first=True,
    )
    sums = call(
        pair_sum_body,
        [struct((64, MODEL), f32)] + [struct((64, MODEL), bf16)] * 3,
        [mine, shift(theirs, "c", 1)],
    )
    got = [shift(sums[s], "x", s) for s in (1, 2, 3)]
    (out,) = call(end_body, [struct((64, MODEL), bf16)], [sums[0], *got, out_gain[None, :]])
    return out


def solution(mesh):
    fine = Mesh(mesh.devices.reshape(8, 4, 4, 2), ("z", "y", "x", "c"))
    sp, tp = ("z", "y"), ("x", "c")
    return jax.shard_map(
        local,
        mesh=fine,
        in_specs=(
            P(sp, tp),
            P(),
            P(None, tp),
            P(None, tp),
            P(None, tp),
            P(tp),
            P(),
            P(),
            P(),
            P(),
            P(),
            P(None, tp),
            P(None, tp),
            P(None, tp),
            P(None, tp),
            P(tp, None),
            P(tp, None),
            P(),
        ),
        out_specs=P(("z", "y", "x", "c"), None),
        check_vma=False,
    )
```
